32 devices in a mesh: sp: 8 (over z, y), tp: 4 (over x, core).
Axes of the slice: x: 2, y: 2, z: 4, core: 2. Of those that a mesh axis runs over, the one named last changes fastest.
Arguments:
- latents: bfloat16 [5120, 2048], P('sp'), may hold values from -6 to 6
- cond: float32 [2048], replicated, may hold values from -6 to 6
- ctx_cond: float32 [2048], replicated, may hold values from -6 to 6
- context: bfloat16 [768, 2048], P('sp'), may hold values from -6 to 6
- norm_gain: float32 [2048], replicated, may hold values from 0.1 to 1.9
- shift_weight: bfloat16 [2048, 2048], P('tp'), may hold values from -0.125 to 0.125
- scale_weight: bfloat16 [2048, 2048], P('tp'), may hold values from -0.125 to 0.125
- gate_weight: bfloat16 [2048, 2048], P('tp'), may hold values from -0.125 to 0.125
- q_weight: bfloat16 [2048, 1024], P(None, 'tp'), may hold values from -0.125 to 0.125
- k_weight: bfloat16 [2048, 1024], P(None, 'tp'), may hold values from -0.125 to 0.125
- v_weight: bfloat16 [2048, 1024], P(None, 'tp'), may hold values from -0.125 to 0.125
- out_weight: bfloat16 [1024, 2048], replicated, may hold values from -1.5 to 1.5
- rel_bias: float32 [8, 15, 31], P('tp'), may hold values from 1.5 to 260
Outputs:
- result: bfloat16 [5120, 2048], P(('sp', 'tp'))
The draws below stay inside these ranges and needn't reach their ends.
All inputs are finite; a program needn't handle non-finite values.
Results may differ from the reference program's by a relative error of at most 0.0085.
Values may be sent and summed in bfloat16 or wider, within the bound.
A program may use at most 64 MiB of HBM per device.

```python
import jax
import jax.numpy as jnp
from jax import lax

D = 2048
HEADS = 8
HEAD_DIM = 128
GRID_W = 64
WIN_ROWS = 8
WIN_COLS = 16
CTX = 768
ROWS = 80
TOKENS = 5120
NA_WIDTH = 1024


def draw_rel_bias(key, part):
    base_key = jax.random.fold_in(jax.random.fold_in(key, 4711), 0)
    table = jax.random.uniform(base_key, (HEADS, 2 * WIN_ROWS - 1, 2 * WIN_COLS - 1), jnp.float32, 1.5, 4.5)
    return table.astype(jnp.float32)


def block_scale(own_key, extent, cuts, low, top_value):
    def one(axis_at, parts):
        steps = jax.random.uniform(jax.random.fold_in(jax.random.fold_in(own_key, 6), axis_at), (parts,), jnp.float32, low / len(cuts), top_value / len(cuts))
        return jnp.repeat(jnp.exp(steps), extent[axis_at] // parts).reshape((-1,) + (1,) * (len(extent) - axis_at - 1))

    level = one(*cuts[0])
    for cut in cuts[1:]:
        level = level * one(*cut)
    return level


def noise(stream_key, shape, width, limit, cuts=(), kind=jnp.bfloat16):
    level = block_scale(stream_key, shape, cuts, -0.22, 0.18) if cuts else 1.0
    array = jax.random.normal(stream_key, shape, jnp.float32) * width * level
    return jnp.minimum(jnp.maximum(array, -limit), limit).astype(kind)


def setup_inputs(seed: int = 0) -> dict:
    key_list = jax.random.split(jax.random.key(seed), 14)
    return {
        "latents": noise(key_list[0], (TOKENS, D), 1.0, 6.0, ((0, 8),)),
        "cond": noise(key_list[1], (D,), 1.0, 6.0, (), jnp.float32),
        "ctx_cond": noise(key_list[2], (D,), 1.0, 6.0, (), jnp.float32),
        "context": noise(key_list[3], (CTX, D), 1.0, 6.0, ((0, 8),)),
        "norm_gain": jnp.clip(1.0 + 0.18 * jax.random.normal(key_list[4], (D,), jnp.float32), 0.1, 1.9),
        "shift_weight": noise(key_list[5], (D, D), D ** -0.5, 0.125, ((0, 4),)),
        "scale_weight": noise(key_list[6], (D, D), D ** -0.5, 0.125, ((0, 4),)),
        "gate_weight": noise(key_list[7], (D, D), D ** -0.5, 0.125, ((0, 4),)),
        "q_weight": noise(key_list[8], (D, NA_WIDTH), D ** -0.5, 0.125, ((1, 4),)),
        "k_weight": noise(key_list[9], (D, NA_WIDTH), D ** -0.5, 0.125, ((1, 4),)),
        "v_weight": noise(key_list[10], (D, NA_WIDTH), D ** -0.5, 0.125, ((1, 4),)),
        "out_weight": noise(key_list[11], (NA_WIDTH, D), (max(NA_WIDTH // 64, 1)) ** -0.5, 1.5),
        "rel_bias": draw_rel_bias(jax.random.fold_in(key_list[13], 71), 0),
    }


EPS = 1e-06
NEG_BIG = -1e+30

def modulated_norm(tok_rows, gain, shift_row, scale_row):
    rows_f = tok_rows.astype(jnp.float32)
    inverse = lax.rsqrt(lax.optimization_barrier(jnp.mean(rows_f * rows_f, axis=-1, keepdims=True)) + EPS)
    return (rows_f * inverse * gain * (1.0 + scale_row) + shift_row).astype(jnp.bfloat16)

def column_mask():
    columns = jnp.arange(GRID_W, dtype=jnp.int32)
    first_col = jnp.clip(columns - WIN_COLS // 2, 0, GRID_W - WIN_COLS)
    inside = (columns[None, :] >= first_col[:, None]) & (columns[None, :] < first_col[:, None] + WIN_COLS)
    return jnp.tile(inside, (1, WIN_ROWS))

def grid_bias(bias_table, row_diff):
    row_hot = (row_diff[:, :, None] == jnp.arange(2 * WIN_ROWS - 1, dtype=jnp.int32)[None, None, :]).astype(jnp.float32)
    columns = jnp.arange(GRID_W, dtype=jnp.int32)
    col_diff = jnp.clip(columns[None, :] - columns[:, None], -(WIN_COLS - 1), WIN_COLS - 1) + WIN_COLS - 1
    col_hot = (col_diff[:, :, None] == jnp.arange(2 * WIN_COLS - 1, dtype=jnp.int32)[None, None, :]).astype(jnp.float32)
    middle = jnp.einsum('rai,hij->hraj', row_hot, bias_table.astype(jnp.float32), precision=lax.Precision.HIGHEST)
    spread = jnp.einsum('hraj,qbj->hrqab', middle, col_hot, precision=lax.Precision.HIGHEST)
    return spread.reshape(bias_table.shape[0], row_diff.shape[0], GRID_W, WIN_ROWS * GRID_W)

def attend(query, key_win, val_win, ctx_keys, ctx_vals, bias, inside):
    factor = HEAD_DIM ** (-0.5)
    near_scores = jnp.einsum('rqhd,rkhd->hrqk', query.astype(jnp.float32), key_win.astype(jnp.float32)) * factor + bias
    near_scores = jnp.where(inside, near_scores, NEG_BIG)
    far_scores = jnp.einsum('rqhd,lhd->hrql', query.astype(jnp.float32), ctx_keys.astype(jnp.float32)) * factor
    row_peak = jnp.maximum(lax.optimization_barrier(jnp.max(near_scores, axis=-1, keepdims=True)), lax.optimization_barrier(jnp.max(far_scores, axis=-1, keepdims=True)))
    near_exp = jnp.exp(near_scores - row_peak)
    far_exp = jnp.exp(far_scores - row_peak)
    denominator = lax.optimization_barrier(jnp.sum(near_exp, axis=-1, keepdims=True)) + lax.optimization_barrier(jnp.sum(far_exp, axis=-1, keepdims=True))
    near_w = (near_exp / denominator).astype(jnp.bfloat16)
    far_w = (far_exp / denominator).astype(jnp.bfloat16)
    mixed = jnp.einsum('hrqk,rkhd->rqhd', near_w.astype(jnp.float32), val_win.astype(jnp.float32)) + jnp.einsum('hrql,lhd->rqhd', far_w.astype(jnp.float32), ctx_vals.astype(jnp.float32))
    return mixed.astype(jnp.bfloat16)

def reference(latents, cond, ctx_cond, context, norm_gain, shift_weight, scale_weight, gate_weight, q_weight, k_weight, v_weight, out_weight, rel_bias):
    conds = jnp.stack([cond, ctx_cond])
    active = jax.nn.silu(conds).astype(jnp.bfloat16)
    shifts = jnp.dot(active, shift_weight, preferred_element_type=jnp.float32)
    scales = jnp.dot(active, scale_weight, preferred_element_type=jnp.float32)
    gates = jnp.dot(active[:1], gate_weight, preferred_element_type=jnp.float32)
    h_lat = modulated_norm(latents, norm_gain, shifts[0], scales[0])
    h_ctx = modulated_norm(context, norm_gain, shifts[1], scales[1])
    query = jnp.dot(h_lat, q_weight, preferred_element_type=jnp.float32).astype(jnp.bfloat16)
    keys = jnp.dot(h_lat, k_weight, preferred_element_type=jnp.float32).astype(jnp.bfloat16)
    values = jnp.dot(h_lat, v_weight, preferred_element_type=jnp.float32).astype(jnp.bfloat16)
    ctx_keys = jnp.dot(h_ctx, k_weight, preferred_element_type=jnp.float32).astype(jnp.bfloat16)
    ctx_vals = jnp.dot(h_ctx, v_weight, preferred_element_type=jnp.float32).astype(jnp.bfloat16)
    grid_rows = jnp.arange(ROWS, dtype=jnp.int32)
    first_row = jnp.clip(grid_rows - WIN_ROWS // 2, 0, ROWS - WIN_ROWS)
    offsets = jnp.arange(WIN_ROWS, dtype=jnp.int32)
    row_index = first_row[:, None] + offsets[None, :]
    row_diff = row_index - grid_rows[:, None] + WIN_ROWS - 1
    inside = column_mask()
    query_grid = query.reshape(ROWS, GRID_W, HEADS, HEAD_DIM)
    key_grid = keys.reshape(ROWS, GRID_W, HEADS, HEAD_DIM)
    val_grid = values.reshape(ROWS, GRID_W, HEADS, HEAD_DIM)
    ctx_key3 = ctx_keys.reshape(CTX, HEADS, HEAD_DIM)
    ctx_val3 = ctx_vals.reshape(CTX, HEADS, HEAD_DIM)

    def one_head(head_id):
        query_head = lax.dynamic_slice_in_dim(query_grid, head_id, 1, 2)
        key_head = lax.dynamic_slice_in_dim(key_grid, head_id, 1, 2)[row_index]
        val_head = lax.dynamic_slice_in_dim(val_grid, head_id, 1, 2)[row_index]
        key_head = key_head.reshape(ROWS, WIN_ROWS * GRID_W, 1, HEAD_DIM)
        val_head = val_head.reshape(ROWS, WIN_ROWS * GRID_W, 1, HEAD_DIM)
        ctx_key_head = lax.dynamic_slice_in_dim(ctx_key3, head_id, 1, 1)
        ctx_val_head = lax.dynamic_slice_in_dim(ctx_val3, head_id, 1, 1)
        bias = grid_bias(lax.dynamic_slice_in_dim(rel_bias, head_id, 1, 0), row_diff)
        return attend(query_head, key_head, val_head, ctx_key_head, ctx_val_head, bias, inside)
    head_outs = lax.map(one_head, jnp.arange(HEADS, dtype=jnp.int32))
    attn = jnp.transpose(head_outs[:, :, :, 0], (1, 2, 0, 3)).reshape(TOKENS, NA_WIDTH)
    mixed = jnp.dot(attn, out_weight, preferred_element_type=jnp.float32)
    return (latents.astype(jnp.float32) + gates[0] * mixed).astype(jnp.bfloat16)
```

```python
import functools

import jax
import jax.numpy as jnp
from jax import lax
from jax.experimental import pallas as pl
from jax.experimental.pallas import tpu as pltpu
from jax.sharding import PartitionSpec as P

HEAD_DIM = 128
GRID_W = 64
WIN_ROWS = 8
WIN_COLS = 16
EPS = 1e-06
NEG_BIG = -1e30
F32 = jnp.float32
BF16 = jnp.bfloat16
UP_ROWS = WIN_ROWS // 2
DOWN_ROWS = WIN_ROWS // 2 - 1
TILE = 128
PAIR = 2 * GRID_W


def dot(a, b):
    return jnp.dot(a, b, preferred_element_type=F32)


def dot_t(a, b):
    return lax.dot_general(a, b, (((1,), (1,)), ((), ())), preferred_element_type=F32)


def kernel(
    ns, nt,
    conds, gain, table,
    lat_h, ctx_h, wsh_h, wsc_h, wg_h, wq_h, wk_h, wv_h, wo_h,
    out,
    lat, ctx, wsh, wsc, wg, wqkv, wo,
    modr, gater, mods, ctx_all, kv, q, bias, o_far, m_far, l_far, att, own,
    load_sem, mod_s, mod_r, gate_s, gate_r, ctx_s, ctx_r, halo_s, halo_r, head_s, head_r,
):
    sp, tp = lax.axis_index("sp"), lax.axis_index("tp")
    tokens, d = lat.shape
    c_here = ctx.shape[0]
    width = q.shape[1]
    heads = width // HEAD_DIM
    kt = wsh.shape[0]
    rows = tokens // GRID_W
    total_rows = rows * ns
    own_n = tokens // nt
    up_n, down_n = UP_ROWS * GRID_W, DOWN_ROWS * GRID_W
    factor = HEAD_DIM ** -0.5

    loads = [
        pltpu.make_async_copy(s, t, load_sem.at[i])
        for i, (s, t) in enumerate([
            (wsh_h, wsh), (wsc_h, wsc), (ctx_h, ctx),
            (wk_h, wqkv.at[:, pl.ds(0, width)]), (wv_h, wqkv.at[:, pl.ds(width, width)]),
            (lat_h, lat), (wq_h, wqkv.at[:, pl.ds(2 * width, width)]), (wg_h, wg), (wo_h, wo),
        ])
    ]
    for c in loads:
        c.start()

    barrier = pltpu.get_barrier_semaphore()

    def greet_tp(o, _):
        pl.semaphore_signal(barrier, inc=1, device_id={"sp": sp, "tp": (tp + o) % nt})
        return 0

    def greet_sp(o, _):
        pl.semaphore_signal(barrier, inc=1, device_id={"sp": (sp + o) % ns, "tp": tp})
        return 0

    lax.fori_loop(1, nt, greet_tp, 0)
    lax.fori_loop(1, ns, greet_sp, 0)

    start = pl.multiple_of(tp * kt, 128)
    v = conds[:, pl.ds(start, kt)]
    act = v / (1.0 + jnp.exp(-v))
    row = lax.broadcasted_iota(jnp.int32, (8, kt), 0)
    mixed_act, row0_act = act[:8], act[8:]

    def only(a, keep):
        return jnp.where(keep, a, 0.0).astype(BF16)

    loads[0].wait()
    loads[1].wait()
    half_d = d // 2
    a_sh = [only(mixed_act, (row // 2) == 2 * k) for k in range(2)]
    a_sc = [only(mixed_act, (row // 2) == 2 * k + 1) for k in range(2)]
    step = 512
    for n0 in range(0, half_d, step):
        part = jnp.zeros((8, step), F32)
        for k in range(2):
            cols = pl.ds(k * half_d + n0, step)
            part = part + dot(a_sh[k], wsh[:, cols]) + dot(a_sc[k], wsc[:, cols])
        modr[tp, :, pl.ds(n0, step)] = part
    pl.semaphore_wait(barrier, nt - 1 + ns - 1)

    def tp_copy(buf, s_sem, r_sem, o):
        return pltpu.make_async_remote_copy(
            src_ref=buf.at[tp], dst_ref=buf.at[tp],
            send_sem=s_sem.at[o], recv_sem=r_sem.at[o],
            device_id={"sp": sp, "tp": (tp + o) % nt},
        )

    def start_mod(o, _):
        tp_copy(modr, mod_s, mod_r, o).start()
        return 0

    lax.fori_loop(1, nt, start_mod, 0)

    qc = lax.broadcasted_iota(jnp.int32, (GRID_W, PAIR), 0)
    kc = lax.broadcasted_iota(jnp.int32, (GRID_W, PAIR), 1) % GRID_W
    first = jnp.clip(qc - WIN_COLS // 2, 0, GRID_W - WIN_COLS)
    inside = (kc >= first) & (kc < first + WIN_COLS)
    for h in range(heads):
        for i in range(2 * WIN_ROWS - 2):
            line = jnp.broadcast_to(table[h, pl.ds(i, 1), :], (GRID_W, PAIR))
            rolled = pltpu.roll(line, 0, 1, stride=1, stride_axis=0)
            bias[h, i] = jnp.where(inside, rolled, NEG_BIG)

    loads[7].wait()
    seg = d // 8
    gp = jnp.zeros((8, seg), F32)
    for j in range(8):
        gp = gp + dot(only(row0_act, row == j), wg[:, pl.ds(j * seg, seg)])
    gater[tp] = gp

    def start_gate(o, _):
        tp_copy(gater, gate_s, gate_r, o).start()
        return 0

    lax.fori_loop(1, nt, start_gate, 0)

    def wait_mod(o, _):
        tp_copy(modr, mod_s, mod_r, o).wait()
        return 0

    lax.fori_loop(1, nt, wait_mod, 0)
    total = modr[0]
    for i in range(1, nt):
        total = total + modr[i]
    g = gain[...]
    for k in range(2):
        cols = pl.ds(k * half_d, half_d)
        gk = g[:, k * half_d:(k + 1) * half_d]
        mods[0:1, cols] = gk * (1.0 + total[4 * k + 2:4 * k + 3])
        mods[1:2, cols] = total[4 * k:4 * k + 1]
        mods[2:3, cols] = gk * (1.0 + total[4 * k + 3:4 * k + 4])
        mods[3:4, cols] = total[4 * k + 1:4 * k + 2]

    def norm(x, r):
        xf = x.astype(F32)
        inv = lax.rsqrt(jnp.mean(xf * xf, axis=-1, keepdims=True) + EPS)
        return (xf * inv * mods[r:r + 1, :] + mods[r + 1:r + 2, :]).astype(BF16)

    loads[2].wait()
    loads[3].wait()
    loads[4].wait()
    ctx_all[sp] = dot(norm(ctx[...], 2), wqkv[:, 0:2 * width]).astype(BF16)

    def ctx_copy(o):
        return pltpu.make_async_remote_copy(
            src_ref=ctx_all.at[sp], dst_ref=ctx_all.at[sp],
            send_sem=ctx_s.at[o], recv_sem=ctx_r.at[o],
            device_id={"sp": (sp + o) % ns, "tp": tp},
        )

    def start_ctx(o, _):
        ctx_copy(o).start()
        return 0

    lax.fori_loop(1, ns, start_ctx, 0)

    up = pltpu.make_async_remote_copy(
        src_ref=kv.at[pl.ds(tokens, up_n)], dst_ref=kv.at[pl.ds(0, up_n)],
        send_sem=halo_s.at[0], recv_sem=halo_r.at[0],
        device_id={"sp": (sp + 1) % ns, "tp": tp},
    )
    down = pltpu.make_async_remote_copy(
        src_ref=kv.at[pl.ds(up_n, down_n)], dst_ref=kv.at[pl.ds(up_n + tokens, down_n)],
        send_sem=halo_s.at[1], recv_sem=halo_r.at[1],
        device_id={"sp": (sp + ns - 1) % ns, "tp": tp},
    )
    has_next, has_prev = sp < ns - 1, sp > 0

    loads[5].wait()
    loads[6].wait()
    tiles = tokens // TILE
    up_tiles = pl.cdiv(up_n, TILE)
    down_tiles = pl.cdiv(down_n, TILE)

    def project(s, _):
        t = jnp.where(s < up_tiles, tiles - 1 - s, s - up_tiles)
        base = pl.multiple_of(t * TILE, TILE)
        h = norm(lat[pl.ds(base, TILE), :], 0)
        r = dot(h, wqkv[...]).astype(BF16)
        kv[pl.ds(base + up_n, TILE), :] = r[:, :2 * width]
        q[pl.ds(base, TILE), :] = r[:, 2 * width:]

        @pl.when((s == up_tiles - 1) & has_next)
        def _():
            up.start()

        @pl.when((s == up_tiles + down_tiles - 1) & has_prev)
        def _():
            down.start()

        return 0

    lax.fori_loop(0, tiles, project, 0)

    def wait_ctx(o, _):
        ctx_copy(o).wait()
        return 0

    lax.fori_loop(1, ns, wait_ctx, 0)

    def flat(x):
        if c_here % 16:
            return x.astype(F32).reshape(ns * c_here, HEAD_DIM).astype(BF16)
        return x.reshape(ns * c_here, HEAD_DIM)

    for h in range(heads):
        lo = h * HEAD_DIM
        ck = flat(ctx_all[:, :, lo:lo + HEAD_DIM])
        cv = flat(ctx_all[:, :, width + lo:width + lo + HEAD_DIM])

        def far(t, _):
            ids = pl.ds(pl.multiple_of(t * TILE, TILE), TILE)
            s = dot_t(q[ids, lo:lo + HEAD_DIM], ck) * factor
            m = jnp.max(s, axis=-1, keepdims=True)
            e = jnp.exp(s - m)
            l_far[h, ids, :] = jnp.sum(e, axis=-1, keepdims=True)
            m_far[h, ids, :] = m
            o_far[ids, lo:lo + HEAD_DIM] = dot(e.astype(BF16), cv)
            return 0

        lax.fori_loop(0, tiles, far, 0)

    @pl.when(has_next)
    def _():
        up.wait_send()

    @pl.when(has_prev)
    def _():
        down.wait_send()
        up.wait_recv()

    @pl.when(has_next)
    def _():
        down.wait_recv()

    half_t = nt // 2
    half_rows = rows // 2
    my_half = tp // half_t
    base_row = sp * rows

    def near(i, r0):
        r = r0 + i
        grid_row = base_row + r
        s_row = jnp.clip(grid_row - WIN_ROWS // 2, 0, total_rows - WIN_ROWS)
        i0 = s_row - grid_row + WIN_ROWS - 1
        win = pl.ds(pl.multiple_of((s_row - base_row + UP_ROWS) * GRID_W, GRID_W), WIN_ROWS * GRID_W)
        ids = pl.ds(pl.multiple_of(r * GRID_W, GRID_W), GRID_W)
        for h in range(heads):
            lo = h * HEAD_DIM
            b = jnp.concatenate([bias[h, i0 + 2 * k] for k in range(WIN_ROWS // 2)], axis=1)
            s = dot_t(q[ids, lo:lo + HEAD_DIM], kv[win, lo:lo + HEAD_DIM]) * factor + b
            mf = m_far[h, ids, :]
            m = jnp.maximum(jnp.max(s, axis=-1, keepdims=True), mf)
            e = jnp.exp(s - m)
            w = jnp.exp(mf - m)
            l = jnp.sum(e, axis=-1, keepdims=True) + w * l_far[h, ids, :]
            o = dot(e.astype(BF16), kv[win, width + lo:width + lo + HEAD_DIM])
            o = (o + w * o_far[ids, lo:lo + HEAD_DIM]) / l
            att[ids, lo:lo + HEAD_DIM] = o.astype(BF16)
        return r0

    def head_copy(src, dst):
        return pltpu.make_async_remote_copy(
            src_ref=att.at[pl.ds(pl.multiple_of(dst * own_n, 16), own_n)], dst_ref=own.at[src],
            send_sem=head_s.at[dst], recv_sem=head_r.at[src],
            device_id={"sp": sp, "tp": dst},
        )

    lax.fori_loop(0, half_rows, near, (1 - my_half) * half_rows)

    def send_other(j, _):
        head_copy(tp, (1 - my_half) * half_t + j).start()
        return 0

    lax.fori_loop(0, half_t, send_other, 0)
    lax.fori_loop(0, half_rows, near, my_half * half_rows)

    def mate(o):
        return my_half * half_t + (tp + o) % half_t

    def send_same(o, _):
        head_copy(tp, mate(o)).start()
        return 0

    lax.fori_loop(1, half_t, send_same, 0)

    def wait_gate(o, _):
        tp_copy(gater, gate_s, gate_r, o).wait()
        return 0

    lax.fori_loop(1, nt, wait_gate, 0)
    gsum = gater[0]
    for i in range(1, nt):
        gsum = gsum + gater[i]
    gates = jnp.concatenate([gsum[j:j + 1] for j in range(8)], axis=1)
    loads[8].wait()
    own[tp] = att[pl.ds(pl.multiple_of(tp * own_n, 16), own_n), :]

    def settle(o, _):
        p = (tp + o) % nt
        head_copy(tp, p).wait_send()
        head_copy(p, p).wait_recv()
        return 0

    lax.fori_loop(1, nt, settle, 0)
    a = jnp.concatenate([own[i] for i in range(nt)], axis=1)
    my_rows = pl.ds(pl.multiple_of(tp * own_n, 16), own_n)
    for n0 in range(0, d, 512):
        y = dot(a, wo[:, n0:n0 + 512])
        out[:, n0:n0 + 512] = (
            lat[my_rows, n0:n0 + 512].astype(F32) + gates[:, n0:n0 + 512] * y
        ).astype(BF16)


def shards(
    ns, nt,
    latents, cond, ctx_cond, context, norm_gain, shift_weight, scale_weight, gate_weight,
    q_weight, k_weight, v_weight, out_weight, rel_bias,
):
    tokens, d = latents.shape
    c_here = context.shape[0]
    kt = shift_weight.shape[0]
    width = q_weight.shape[1]
    heads = width // HEAD_DIM
    own_n = tokens // nt
    conds = jnp.stack([cond, ctx_cond] * 4 + [cond] * 8)
    here, after = rel_bias[:, :-1], rel_bias[:, 1:]
    reach = WIN_COLS - 1
    gap = jnp.zeros(here.shape[:2] + (GRID_W - 2 * reach - 1,), F32)
    table = jnp.concatenate([here[..., reach:], gap, after, gap, here[..., :reach]], axis=-1)
    halo = (UP_ROWS + DOWN_ROWS) * GRID_W
    vmem = pl.BlockSpec(memory_space=pltpu.VMEM)
    hbm = pl.BlockSpec(memory_space=pl.ANY)
    sem = pltpu.SemaphoreType.DMA
    return pl.pallas_call(
        functools.partial(kernel, ns, nt),
        out_shape=jax.ShapeDtypeStruct((own_n, d), BF16),
        in_specs=[vmem] * 3 + [hbm] * 9,
        out_specs=vmem,
        scratch_shapes=[
            pltpu.VMEM((tokens, d), BF16),
            pltpu.VMEM((c_here, d), BF16),
            pltpu.VMEM((kt, d), BF16),
            pltpu.VMEM((kt, d), BF16),
            pltpu.VMEM((kt, d), BF16),
            pltpu.VMEM((d, 3 * width), BF16),
            pltpu.VMEM(out_weight.shape, BF16),
            pltpu.VMEM((nt, 8, d // 2), F32),
            pltpu.VMEM((nt, 8, d // 8), F32),
            pltpu.VMEM((8, d), F32),
            pltpu.VMEM((ns, c_here, 2 * width), BF16),
            pltpu.VMEM((tokens + halo, 2 * width), BF16),
            pltpu.VMEM((tokens, width), BF16),
            pltpu.VMEM((heads, 2 * WIN_ROWS - 2, GRID_W, PAIR), F32),
            pltpu.VMEM((tokens, width), F32),
            pltpu.VMEM((heads, tokens, 1), F32),
            pltpu.VMEM((heads, tokens, 1), F32),
            pltpu.VMEM((tokens, width), BF16),
            pltpu.VMEM((nt, own_n, width), BF16),
            sem((9,)),
            sem((nt,)), sem((nt,)), sem((nt,)), sem((nt,)),
            sem((ns,)), sem((ns,)),
            sem((2,)), sem((2,)),
            sem((nt,)), sem((nt,)),
        ],
        compiler_params=pltpu.CompilerParams(
            collective_id=0, has_side_effects=True, vmem_limit_bytes=62 * 1024 * 1024
        ),
    )(
        conds, norm_gain[None], table, latents, context, shift_weight, scale_weight, gate_weight,
        q_weight, k_weight, v_weight, out_weight,
    )


def solution(mesh):
    in_specs = (
        P("sp", None),
        P(),
        P(),
        P("sp", None),
        P(),
        P("tp", None),
        P("tp", None),
        P("tp", None),
        P(None, "tp"),
        P(None, "tp"),
        P(None, "tp"),
        P(),
        P("tp", None, None),
    )
    body = functools.partial(shards, mesh.shape["sp"], mesh.shape["tp"])
    return jax.shard_map(
        body, mesh=mesh, in_specs=in_specs, out_specs=P(("sp", "tp"), None), check_vma=False
    )
```

```python
import functools

import jax
import jax.numpy as jnp
from jax import lax
from jax.experimental import pallas as pl
from jax.experimental.pallas import tpu as pltpu
from jax.sharding import PartitionSpec as P

HEAD_DIM = 128
GRID_W = 64
WIN_ROWS = 8
WIN_COLS = 16
EPS = 1e-06
NEG_BIG = -1e30
F32 = jnp.float32
BF16 = jnp.bfloat16
UP_ROWS = WIN_ROWS // 2
DOWN_ROWS = WIN_ROWS // 2 - 1
TILE = 128
PAIR = 2 * GRID_W
VMEM_BYTES = 67043328


def dot(a, b):
    return jnp.dot(a, b, preferred_element_type=F32)


def dot_t(a, b):
    return lax.dot_general(a, b, (((1,), (1,)), ((), ())), preferred_element_type=F32)


def kernel(
    ns, nt, ny,
    cond, ctx_cond, gain, table,
    lat_h, ctx_h, wsh_h, wsc_h, wg_h, wq_h, wk_h, wv_h, wo_h,
    out,
    lat, ctx, wsh, wsc, wg, wqkv, wo,
    modr, gater, mods, ctx_all, kv, q, bias, o_near, m_near, l_near, att, own, lines,
    load_sem, mod_s, mod_r, gate_s, gate_r, ctx_s, ctx_r, halo_s, halo_r, head_s, head_r,
):
    sp, tp = lax.axis_index("sp"), lax.axis_index("tp")
    tokens, d = lat.shape
    c_here = ctx.shape[0]
    width = q.shape[1]
    heads = width // HEAD_DIM
    kt = wsh.shape[0]
    rows = tokens // GRID_W
    total_rows = rows * ns
    own_n = tokens // nt
    up_n, down_n = UP_ROWS * GRID_W, DOWN_ROWS * GRID_W
    to_log2 = 1.4426950408889634
    q_scale = HEAD_DIM ** -0.5 * to_log2

    loads = [
        pltpu.make_async_copy(s, t, load_sem.at[i])
        for i, (s, t) in enumerate([
            (wsh_h, wsh), (wsc_h, wsc), (ctx_h, ctx),
            (wk_h, wqkv.at[:, pl.ds(0, width)]), (wv_h, wqkv.at[:, pl.ds(width, width)]),
            (lat_h, lat), (wq_h, wqkv.at[:, pl.ds(2 * width, width)]), (wg_h, wg), (wo_h, wo),
        ])
    ]
    for c in loads:
        c.start()

    barrier = pltpu.get_barrier_semaphore()

    def greet_tp(o, _):
        pl.semaphore_signal(barrier, inc=1, device_id={"sp": sp, "tp": (tp + o) % nt})
        return 0

    def greet_sp(o, _):
        pl.semaphore_signal(barrier, inc=1, device_id={"sp": (sp + o) % ns, "tp": tp})
        return 0

    lax.fori_loop(1, nt, greet_tp, 0)
    lax.fori_loop(1, ns, greet_sp, 0)

    start = pl.multiple_of(tp * kt, 128)
    row = lax.broadcasted_iota(jnp.int32, (8, kt), 0)

    def silu(ref):
        v = ref[:, pl.ds(start, kt)]
        return jnp.broadcast_to(v / (1.0 + jnp.exp(-v)), (8, kt))

    row0_act = silu(cond)
    mixed_act = jnp.where(row % 2 == 0, row0_act, silu(ctx_cond))

    def only(a, keep):
        return jnp.where(keep, a, 0.0).astype(BF16)

    loads[0].wait()
    loads[1].wait()
    half_d = d // 2
    a_sh = [only(mixed_act, (row // 2) == 2 * k) for k in range(2)]
    a_sc = [only(mixed_act, (row // 2) == 2 * k + 1) for k in range(2)]
    step = 512
    for n0 in range(0, half_d, step):
        part = jnp.zeros((8, step), F32)
        for k in range(2):
            cols = pl.ds(k * half_d + n0, step)
            part = part + dot(a_sh[k], wsh[:, cols]) + dot(a_sc[k], wsc[:, cols])
        modr[tp, :, pl.ds(n0, step)] = part
    pl.semaphore_wait(barrier, nt - 1 + ns - 1)

    def tp_copy(buf, s_sem, r_sem, o):
        return pltpu.make_async_remote_copy(
            src_ref=buf.at[tp], dst_ref=buf.at[tp],
            send_sem=s_sem.at[o], recv_sem=r_sem.at[o],
            device_id={"sp": sp, "tp": (tp + o) % nt},
        )

    def start_mod(o, _):
        tp_copy(modr, mod_s, mod_r, o).start()
        return 0

    lax.fori_loop(1, nt, start_mod, 0)

    qc = lax.broadcasted_iota(jnp.int32, (GRID_W, PAIR), 0)
    kc = lax.broadcasted_iota(jnp.int32, (GRID_W, PAIR), 1) % GRID_W
    first = jnp.clip(qc - WIN_COLS // 2, 0, GRID_W - WIN_COLS)
    inside = (kc >= first) & (kc < first + WIN_COLS)
    lines[...] = jnp.zeros_like(lines)
    lines[:, :, 0:2 * WIN_COLS - 1] = table[...]
    for h in range(heads):
        for i in range(2 * WIN_ROWS - 2):
            near_line = jnp.broadcast_to(lines[i, h:h + 1, :], (GRID_W, PAIR))
            next_line = jnp.broadcast_to(lines[i + 1, h:h + 1, :], (GRID_W, PAIR))
            reach = WIN_COLS - 1
            rolled = pltpu.roll(near_line, PAIR - reach, 1, stride=1, stride_axis=0)
            rolled = rolled + pltpu.roll(next_line, GRID_W - reach, 1, stride=1, stride_axis=0)
            bias[h, i] = jnp.where(inside, rolled * to_log2, NEG_BIG)

    loads[7].wait()
    seg = d // 8
    gp = jnp.zeros((8, seg), F32)
    for j in range(8):
        gp = gp + dot(only(row0_act, row == j), wg[:, pl.ds(j * seg, seg)])
    gater[tp] = gp

    def start_gate(o, _):
        tp_copy(gater, gate_s, gate_r, o).start()
        return 0

    lax.fori_loop(1, nt, start_gate, 0)

    def wait_mod(o, _):
        tp_copy(modr, mod_s, mod_r, o).wait()
        return 0

    lax.fori_loop(1, nt, wait_mod, 0)
    total = modr[0]
    for i in range(1, nt):
        total = total + modr[i]
    g = gain[...]
    for k in range(2):
        cols = pl.ds(k * half_d, half_d)
        gk = g[:, k * half_d:(k + 1) * half_d]
        mods[0:1, cols] = gk * (1.0 + total[4 * k + 2:4 * k + 3])
        mods[1:2, cols] = total[4 * k:4 * k + 1]
        mods[2:3, cols] = gk * (1.0 + total[4 * k + 3:4 * k + 4])
        mods[3:4, cols] = total[4 * k + 1:4 * k + 2]

    def norm(x, r):
        xf = x.astype(F32)
        inv = lax.rsqrt(jnp.mean(xf * xf, axis=-1, keepdims=True) + EPS)
        return (xf * inv * mods[r:r + 1, :] + mods[r + 1:r + 2, :]).astype(BF16)

    loads[2].wait()
    loads[3].wait()
    loads[4].wait()
    ctx_all[sp] = dot(norm(ctx[...], 2), wqkv[:, 0:2 * width]).astype(BF16)

    nz = ns // ny
    zi, yi = sp // ny, sp % ny

    def ctx_copy(block, dest, lane):
        return pltpu.make_async_remote_copy(
            src_ref=ctx_all.at[block], dst_ref=ctx_all.at[block],
            send_sem=ctx_s.at[lane, block // ny], recv_sem=ctx_r.at[block],
            device_id={"sp": dest, "tp": tp},
        )

    def across(zb, act):
        def one(o, _):
            act(ctx_copy(zb * ny + yi, zi * ny + (yi + o) % ny, 1 + o))
            return 0

        lax.fori_loop(1, ny, one, 0)

    def upward(zb, act):
        @pl.when(zi < nz - 1)
        def _():
            act(ctx_copy(zb * ny + yi, sp + ny, 0))

    def downward(zb, act):
        @pl.when(zi > 0)
        def _():
            act(ctx_copy(zb * ny + yi, sp - ny, 1))

    def go(c):
        c.start()

    def sent(c):
        c.wait_send()

    def arrived(block):
        ctx_copy(block, sp, 0).wait_recv()

    def relay(k):
        @pl.when(zi - k >= 0)
        def _():
            arrived((zi - k) * ny + yi)
            upward(zi - k, go)
            across(zi - k, go)

        @pl.when(zi + k < nz)
        def _():
            arrived((zi + k) * ny + yi)
            downward(zi + k, go)
            across(zi + k, go)

    upward(zi, go)
    downward(zi, go)
    across(zi, go)

    up = pltpu.make_async_remote_copy(
        src_ref=kv.at[pl.ds(tokens, up_n)], dst_ref=kv.at[pl.ds(0, up_n)],
        send_sem=halo_s.at[0], recv_sem=halo_r.at[0],
        device_id={"sp": (sp + 1) % ns, "tp": tp},
    )
    down = pltpu.make_async_remote_copy(
        src_ref=kv.at[pl.ds(up_n, down_n)], dst_ref=kv.at[pl.ds(up_n + tokens, down_n)],
        send_sem=halo_s.at[1], recv_sem=halo_r.at[1],
        device_id={"sp": (sp + ns - 1) % ns, "tp": tp},
    )
    has_next, has_prev = sp < ns - 1, sp > 0

    loads[5].wait()
    loads[6].wait()
    tiles = tokens // TILE
    up_tiles = pl.cdiv(up_n, TILE)
    down_tiles = pl.cdiv(down_n, TILE)

    def project(s, _):
        t = jnp.where(s < up_tiles, tiles - 1 - s, s - up_tiles)
        base = pl.multiple_of(t * TILE, TILE)
        h = norm(lat[pl.ds(base, TILE), :], 0)
        r = dot(h, wqkv[...])
        kv[pl.ds(base + up_n, TILE), :] = r[:, :2 * width].astype(BF16)
        q[pl.ds(base, TILE), :] = (r[:, 2 * width:] * q_scale).astype(BF16)

        @pl.when((s == up_tiles - 1) & has_next)
        def _():
            up.start()

        @pl.when((s == up_tiles + down_tiles - 1) & has_prev)
        def _():
            down.start()

        return 0

    lax.fori_loop(0, tiles, project, 0)

    half_t = nt // 2
    my_half = tp // half_t
    base_row = sp * rows

    def near(i, r0):
        r = r0 + i
        grid_row = base_row + r
        s_row = jnp.clip(grid_row - WIN_ROWS // 2, 0, total_rows - WIN_ROWS)
        i0 = s_row - grid_row + WIN_ROWS - 1
        win = pl.ds(pl.multiple_of((s_row - base_row + UP_ROWS) * GRID_W, GRID_W), WIN_ROWS * GRID_W)
        ids = pl.ds(pl.multiple_of(r * GRID_W, GRID_W), GRID_W)
        for h in range(heads):
            lo = h * HEAD_DIM
            b = jnp.concatenate([bias[h, i0 + 2 * k] for k in range(WIN_ROWS // 2)], axis=1)
            s = dot_t(q[ids, lo:lo + HEAD_DIM], kv[win, lo:lo + HEAD_DIM]) + b
            m = jnp.max(s, axis=-1, keepdims=True)
            e = jnp.exp2(s - m)
            l_near[h, ids, :] = jnp.sum(e, axis=-1, keepdims=True)
            m_near[h, ids, :] = m
            o_near[ids, lo:lo + HEAD_DIM] = dot(
                e.astype(BF16), kv[win, width + lo:width + lo + HEAD_DIM]
            )
        return r0

    relay(1)
    mid = rows - UP_ROWS - DOWN_ROWS
    lax.fori_loop(0, mid, near, UP_ROWS, unroll=True)
    if nz > 2:
        relay(2)

    @pl.when(has_next)
    def _():
        down.wait_recv()
        up.wait_send()

    @pl.when(has_prev)
    def _():
        up.wait_recv()
        down.wait_send()

    lax.fori_loop(0, DOWN_ROWS, near, rows - DOWN_ROWS, unroll=True)
    if nz > 3:
        relay(3)
    lax.fori_loop(0, UP_ROWS, near, 0, unroll=True)

    def late_relay(k, _):
        relay(k)
        return 0

    lax.fori_loop(4, nz, late_relay, 0)

    def settle_row(zb, _):
        def other(o, _):
            arrived(zb * ny + (yi + o) % ny)
            return 0

        lax.fori_loop(1, ny, other, 0)
        across(zb, sent)

        @pl.when(zb <= zi)
        def _():
            upward(zb, sent)

        @pl.when(zb >= zi)
        def _():
            downward(zb, sent)

        return 0

    lax.fori_loop(0, nz, settle_row, 0)

    def flat(x):
        if c_here % 16:
            return x.astype(F32).reshape(ns * c_here, HEAD_DIM).astype(BF16)
        return x.reshape(ns * c_here, HEAD_DIM)

    far_tile = tokens // 4

    def far(t):
        ids = pl.ds(pl.multiple_of(t * far_tile, 16), far_tile)
        for h in range(heads):
            lo = h * HEAD_DIM
            ck = flat(ctx_all[:, :, lo:lo + HEAD_DIM])
            cv = flat(ctx_all[:, :, width + lo:width + lo + HEAD_DIM])
            s = dot_t(q[ids, lo:lo + HEAD_DIM], ck)
            mn = m_near[h, ids, :]
            m = jnp.maximum(jnp.max(s, axis=-1, keepdims=True), mn)
            e = jnp.exp2(s - m)
            w = jnp.exp2(mn - m)
            l = jnp.sum(e, axis=-1, keepdims=True) + w * l_near[h, ids, :]
            o = dot(e.astype(BF16), cv) + w * o_near[ids, lo:lo + HEAD_DIM]
            att[ids, lo:lo + HEAD_DIM] = (o / l).astype(BF16)

    def head_copy(src, dst):
        return pltpu.make_async_remote_copy(
            src_ref=att.at[pl.ds(pl.multiple_of(dst * own_n, 16), own_n)], dst_ref=own.at[src],
            send_sem=head_s.at[dst], recv_sem=head_r.at[src],
            device_id={"sp": sp, "tp": dst},
        )

    far((1 - my_half) * 2)
    far((1 - my_half) * 2 + 1)

    def send_other(j, _):
        head_copy(tp, (1 - my_half) * half_t + j).start()
        return 0

    lax.fori_loop(0, half_t, send_other, 0)
    far(my_half * 2)
    far(my_half * 2 + 1)

    def mate(o):
        return my_half * half_t + (tp + o) % half_t

    def send_same(o, _):
        head_copy(tp, mate(o)).start()
        return 0

    lax.fori_loop(1, half_t, send_same, 0)

    def wait_gate(o, _):
        tp_copy(gater, gate_s, gate_r, o).wait()
        return 0

    lax.fori_loop(1, nt, wait_gate, 0)
    gsum = gater[0]
    for i in range(1, nt):
        gsum = gsum + gater[i]
    gates = jnp.concatenate([gsum[j:j + 1] for j in range(8)], axis=1)
    loads[8].wait()
    own[tp] = att[pl.ds(pl.multiple_of(tp * own_n, 16), own_n), :]

    def settle(o, _):
        p = (tp + o) % nt
        head_copy(tp, p).wait_send()
        head_copy(p, p).wait_recv()
        return 0

    lax.fori_loop(1, nt, settle, 0)
    a = jnp.concatenate([own[i] for i in range(nt)], axis=1)
    my_rows = pl.ds(pl.multiple_of(tp * own_n, 16), own_n)
    for n0 in range(0, d, 512):
        y = dot(a, wo[:, n0:n0 + 512])
        out[:, n0:n0 + 512] = (
            lat[my_rows, n0:n0 + 512].astype(F32) + gates[:, n0:n0 + 512] * y
        ).astype(BF16)


def shards(
    ns, nt,
    latents, cond, ctx_cond, context, norm_gain, shift_weight, scale_weight, gate_weight,
    q_weight, k_weight, v_weight, out_weight, rel_bias,
):
    tokens, d = latents.shape
    c_here = context.shape[0]
    kt = shift_weight.shape[0]
    width = q_weight.shape[1]
    heads = width // HEAD_DIM
    own_n = tokens // nt
    table = jnp.transpose(rel_bias, (1, 0, 2))
    ny = 1
    while ns % (2 * ny) == 0 and 4 * ny * ny <= ns:
        ny *= 2
    halo = (UP_ROWS + DOWN_ROWS) * GRID_W
    vmem = pl.BlockSpec(memory_space=pltpu.VMEM)
    hbm = pl.BlockSpec(memory_space=pltpu.HBM)
    sem = pltpu.SemaphoreType.DMA
    return pl.pallas_call(
        functools.partial(kernel, ns, nt, ny),
        out_shape=jax.ShapeDtypeStruct((own_n, d), BF16),
        in_specs=[vmem] * 4 + [hbm] * 9,
        out_specs=vmem,
        scratch_shapes=[
            pltpu.VMEM((tokens, d), BF16),
            pltpu.VMEM((c_here, d), BF16),
            pltpu.VMEM((kt, d), BF16),
            pltpu.VMEM((kt, d), BF16),
            pltpu.VMEM((kt, d), BF16),
            pltpu.VMEM((d, 3 * width), BF16),
            pltpu.VMEM(out_weight.shape, BF16),
            pltpu.VMEM((nt, 8, d // 2), F32),
            pltpu.VMEM((nt, 8, d // 8), F32),
            pltpu.VMEM((8, d), F32),
            pltpu.VMEM((ns, c_here, 2 * width), BF16),
            pltpu.VMEM((tokens + halo, 2 * width), BF16),
            pltpu.VMEM((tokens, width), BF16),
            pltpu.VMEM((heads, 2 * WIN_ROWS - 2, GRID_W, PAIR), F32),
            pltpu.VMEM((tokens, width), F32),
            pltpu.VMEM((heads, tokens, 1), F32),
            pltpu.VMEM((heads, tokens, 1), F32),
            pltpu.VMEM((tokens, width), BF16),
            pltpu.VMEM((nt, own_n, width), BF16),
            pltpu.VMEM((2 * WIN_ROWS - 1, heads, PAIR), F32),
            sem((9,)),
            sem((nt,)), sem((nt,)), sem((nt,)), sem((nt,)),
            sem((ny + 1, ns // ny)), sem((ns,)),
            sem((2,)), sem((2,)),
            sem((nt,)), sem((nt,)),
        ],
        compiler_params=pltpu.CompilerParams(
            collective_id=0, has_side_effects=True, vmem_limit_bytes=VMEM_BYTES - own_n * d * 2 - 300 * 1024
        ),
    )(
        cond[None], ctx_cond[None], norm_gain[None], table, latents, context, shift_weight, scale_weight, gate_weight,
        q_weight, k_weight, v_weight, out_weight,
    )


def solution(mesh):
    in_specs = (
        P("sp", None),
        P(),
        P(),
        P("sp", None),
        P(),
        P("tp", None),
        P("tp", None),
        P("tp", None),
        P(None, "tp"),
        P(None, "tp"),
        P(None, "tp"),
        P(),
        P("tp", None, None),
    )
    body = functools.partial(shards, mesh.shape["sp"], mesh.shape["tp"])
    return jax.shard_map(
        body, mesh=mesh, in_specs=in_specs, out_specs=P(("sp", "tp"), None), check_vma=False
    )
```

```python
import functools

import jax
import jax.numpy as jnp
from jax import lax
from jax.experimental import pallas as pl
from jax.experimental.pallas import tpu as pltpu
from jax.sharding import PartitionSpec as P

HEAD_DIM = 128
GRID_W = 64
WIN_ROWS = 8
WIN_COLS = 16
EPS = 1e-06
NEG_BIG = -1e30
F32 = jnp.float32
BF16 = jnp.bfloat16
UP_ROWS = WIN_ROWS // 2
DOWN_ROWS = WIN_ROWS // 2 - 1
TILE = 128
PAIR = 2 * GRID_W
VMEM_BYTES = 67043328


def dot(a, b):
    return jnp.dot(a, b, preferred_element_type=F32)


def dot_t(a, b):
    return lax.dot_general(a, b, (((1,), (1,)), ((), ())), preferred_element_type=F32)


def kernel(
    ns, nt, ny,
    cond_h, ctx_cond_h, gain_h, table_h,
    lat_h, ctx_h, wsh_h, wsc_h, wg_h, wq_h, wk_h, wv_h, wo_h,
    out,
    lat, ctx, wsh, wsc, wg, wqkv, wo,
    modr, gater, mods, ctx_all, kv, q, bias, o_near, m_near, l_near, att, own, lines,
    cond, ctx_cond, gain, table,
    load_sem, mod_s, mod_r, gate_s, gate_r, ctx_s, ctx_r, halo_s, halo_r, head_s, head_r,
):
    sp, tp = lax.axis_index("sp"), lax.axis_index("tp")
    tokens, d = lat.shape
    c_here = ctx.shape[0]
    width = q.shape[1]
    heads = width // HEAD_DIM
    kt = wsh.shape[0]
    rows = tokens // GRID_W
    total_rows = rows * ns
    own_n = tokens // nt
    up_n, down_n = UP_ROWS * GRID_W, DOWN_ROWS * GRID_W
    to_log2 = 1.4426950408889634
    q_scale = HEAD_DIM ** -0.5 * to_log2

    loads = [
        pltpu.make_async_copy(s, t, load_sem.at[i])
        for i, (s, t) in enumerate([
            (wsh_h, wsh), (wsc_h, wsc), (ctx_h, ctx),
            (wk_h, wqkv.at[:, pl.ds(0, width)]), (wv_h, wqkv.at[:, pl.ds(width, width)]),
            (lat_h, lat), (wq_h, wqkv.at[:, pl.ds(2 * width, width)]), (wg_h, wg), (wo_h, wo),
            (cond_h, cond), (ctx_cond_h, ctx_cond), (gain_h, gain), (table_h, table),
        ])
    ]
    for c in loads[9:] + loads[:9]:
        c.start()

    barrier = pltpu.get_barrier_semaphore()

    def greet_tp(o, _):
        pl.semaphore_signal(barrier, inc=1, device_id={"sp": sp, "tp": (tp + o) % nt})
        return 0

    def greet_sp(o, _):
        pl.semaphore_signal(barrier, inc=1, device_id={"sp": (sp + o) % ns, "tp": tp})
        return 0

    lax.fori_loop(1, nt, greet_tp, 0)
    lax.fori_loop(1, ns, greet_sp, 0)

    for c in loads[9:]:
        c.wait()

    start = pl.multiple_of(tp * kt, 128)
    row = lax.broadcasted_iota(jnp.int32, (8, kt), 0)

    def silu(ref):
        v = ref[:, pl.ds(start, kt)]
        return jnp.broadcast_to(v / (1.0 + jnp.exp(-v)), (8, kt))

    row0_act = silu(cond)
    mixed_act = jnp.where(row % 2 == 0, row0_act, silu(ctx_cond))

    def only(a, keep):
        return jnp.where(keep, a, 0.0).astype(BF16)

    loads[0].wait()
    loads[1].wait()
    half_d = d // 2
    a_sh = [only(mixed_act, (row // 2) == 2 * k) for k in range(2)]
    a_sc = [only(mixed_act, (row // 2) == 2 * k + 1) for k in range(2)]
    step = 512
    for n0 in range(0, half_d, step):
        part = jnp.zeros((8, step), F32)
        for k in range(2):
            cols = pl.ds(k * half_d + n0, step)
            part = part + dot(a_sh[k], wsh[:, cols]) + dot(a_sc[k], wsc[:, cols])
        modr[tp, :, pl.ds(n0, step)] = part
    pl.semaphore_wait(barrier, nt - 1 + ns - 1)

    def tp_copy(buf, s_sem, r_sem, o):
        return pltpu.make_async_remote_copy(
            src_ref=buf.at[tp], dst_ref=buf.at[tp],
            send_sem=s_sem.at[o], recv_sem=r_sem.at[o],
            device_id={"sp": sp, "tp": (tp + o) % nt},
        )

    def start_mod(o, _):
        tp_copy(modr, mod_s, mod_r, o).start()
        return 0

    lax.fori_loop(1, nt, start_mod, 0)

    qc = lax.broadcasted_iota(jnp.int32, (GRID_W, PAIR), 0)
    kc = lax.broadcasted_iota(jnp.int32, (GRID_W, PAIR), 1) % GRID_W
    first = jnp.clip(qc - WIN_COLS // 2, 0, GRID_W - WIN_COLS)
    inside = (kc >= first) & (kc < first + WIN_COLS)
    lines[...] = jnp.zeros_like(lines)
    lines[:, :, 0:2 * WIN_COLS - 1] = table[...]
    for h in range(heads):
        for i in range(2 * WIN_ROWS - 2):
            near_line = jnp.broadcast_to(lines[i, h:h + 1, :], (GRID_W, PAIR))
            next_line = jnp.broadcast_to(lines[i + 1, h:h + 1, :], (GRID_W, PAIR))
            reach = WIN_COLS - 1
            rolled = pltpu.roll(near_line, PAIR - reach, 1, stride=1, stride_axis=0)
            rolled = rolled + pltpu.roll(next_line, GRID_W - reach, 1, stride=1, stride_axis=0)
            bias[h, i] = jnp.where(inside, rolled * to_log2, NEG_BIG)

    def wait_mod(o, _):
        tp_copy(modr, mod_s, mod_r, o).wait()
        return 0

    lax.fori_loop(1, nt, wait_mod, 0)
    total = modr[0]
    for i in range(1, nt):
        total = total + modr[i]
    g = gain[...]
    for k in range(2):
        cols = pl.ds(k * half_d, half_d)
        gk = g[:, k * half_d:(k + 1) * half_d]
        mods[0:1, cols] = gk * (1.0 + total[4 * k + 2:4 * k + 3])
        mods[1:2, cols] = total[4 * k:4 * k + 1]
        mods[2:3, cols] = gk * (1.0 + total[4 * k + 3:4 * k + 4])
        mods[3:4, cols] = total[4 * k + 1:4 * k + 2]

    def norm(x, r):
        xf = x.astype(F32)
        inv = lax.rsqrt(jnp.mean(xf * xf, axis=-1, keepdims=True) + EPS)
        return (xf * inv * mods[r:r + 1, :] + mods[r + 1:r + 2, :]).astype(BF16)

    loads[2].wait()
    loads[3].wait()
    loads[4].wait()
    ctx_all[sp % ny, sp // ny] = dot(norm(ctx[...], 2), wqkv[:, 0:2 * width]).astype(BF16)

    nz = ns // ny
    zi, yi = sp // ny, sp % ny

    def ctx_copy(block, dest, lane):
        return pltpu.make_async_remote_copy(
            src_ref=ctx_all.at[block % ny, block // ny],
            dst_ref=ctx_all.at[block % ny, block // ny],
            send_sem=ctx_s.at[lane, block // ny], recv_sem=ctx_r.at[block],
            device_id={"sp": dest, "tp": tp},
        )

    def across(zb, act):
        def one(o, _):
            act(ctx_copy(zb * ny + yi, zi * ny + (yi + o) % ny, 1 + o))
            return 0

        lax.fori_loop(1, ny, one, 0)

    def upward(zb, act):
        @pl.when(zi < nz - 1)
        def _():
            act(ctx_copy(zb * ny + yi, sp + ny, 0))

    def downward(zb, act):
        @pl.when(zi > 0)
        def _():
            act(ctx_copy(zb * ny + yi, sp - ny, 1))

    def go(c):
        c.start()

    def sent(c):
        c.wait_send()

    def arrived(block):
        ctx_copy(block, sp, 0).wait_recv()

    def relay(k):
        @pl.when(zi - k >= 0)
        def _():
            arrived((zi - k) * ny + yi)
            upward(zi - k, go)
            across(zi - k, go)

        @pl.when(zi + k < nz)
        def _():
            arrived((zi + k) * ny + yi)
            downward(zi + k, go)
            across(zi + k, go)

    upward(zi, go)
    downward(zi, go)
    across(zi, go)

    up = pltpu.make_async_remote_copy(
        src_ref=kv.at[pl.ds(tokens, up_n)], dst_ref=kv.at[pl.ds(0, up_n)],
        send_sem=halo_s.at[0], recv_sem=halo_r.at[0],
        device_id={"sp": (sp + 1) % ns, "tp": tp},
    )
    down = pltpu.make_async_remote_copy(
        src_ref=kv.at[pl.ds(up_n, down_n)], dst_ref=kv.at[pl.ds(up_n + tokens, down_n)],
        send_sem=halo_s.at[1], recv_sem=halo_r.at[1],
        device_id={"sp": (sp + ns - 1) % ns, "tp": tp},
    )
    has_next, has_prev = sp < ns - 1, sp > 0

    loads[5].wait()
    loads[6].wait()
    tiles = tokens // TILE
    up_tiles = pl.cdiv(up_n, TILE)
    down_tiles = pl.cdiv(down_n, TILE)

    def project(s, _):
        t = jnp.where(s < up_tiles, tiles - 1 - s, s - up_tiles)
        base = pl.multiple_of(t * TILE, TILE)
        h = norm(lat[pl.ds(base, TILE), :], 0)
        r = dot(h, wqkv[...])
        kv[pl.ds(base + up_n, TILE), :] = r[:, :2 * width].astype(BF16)
        q[pl.ds(base, TILE), :] = (r[:, 2 * width:] * q_scale).astype(BF16)

        @pl.when((s == up_tiles - 1) & has_next)
        def _():
            up.start()

        @pl.when((s == up_tiles + down_tiles - 1) & has_prev)
        def _():
            down.start()

        return 0

    lax.fori_loop(0, tiles, project, 0)

    loads[7].wait()
    seg = d // 8
    gp = jnp.zeros((8, seg), F32)
    for j in range(8):
        gp = gp + dot(only(row0_act, row == j), wg[:, pl.ds(j * seg, seg)])
    gater[tp] = gp

    def start_gate(o, _):
        tp_copy(gater, gate_s, gate_r, o).start()
        return 0

    lax.fori_loop(1, nt, start_gate, 0)

    half_t = nt // 2
    my_half = tp // half_t
    base_row = sp * rows

    def near(i, r0):
        r = r0 + i
        grid_row = base_row + r
        s_row = jnp.clip(grid_row - WIN_ROWS // 2, 0, total_rows - WIN_ROWS)
        i0 = s_row - grid_row + WIN_ROWS - 1
        win = pl.ds(pl.multiple_of((s_row - base_row + UP_ROWS) * GRID_W, GRID_W), WIN_ROWS * GRID_W)
        ids = pl.ds(pl.multiple_of(r * GRID_W, GRID_W), GRID_W)
        for h in range(heads):
            lo = h * HEAD_DIM
            b = jnp.concatenate([bias[h, i0 + 2 * k] for k in range(WIN_ROWS // 2)], axis=1)
            s = dot_t(q[ids, lo:lo + HEAD_DIM], kv[win, lo:lo + HEAD_DIM]) + b
            m = jnp.max(s, axis=-1, keepdims=True)
            e = jnp.exp2(s - m)
            l_near[h, ids, :] = jnp.sum(e, axis=-1, keepdims=True)
            m_near[h, ids, :] = m
            o_near[ids, lo:lo + HEAD_DIM] = dot(
                e.astype(BF16), kv[win, width + lo:width + lo + HEAD_DIM]
            )
        return r0

    relay(1)
    mid = rows - UP_ROWS - DOWN_ROWS
    lax.fori_loop(0, mid, near, UP_ROWS, unroll=True)
    if nz > 2:
        relay(2)

    @pl.when(has_next)
    def _():
        down.wait_recv()
        up.wait_send()

    @pl.when(has_prev)
    def _():
        up.wait_recv()
        down.wait_send()

    lax.fori_loop(0, DOWN_ROWS, near, rows - DOWN_ROWS, unroll=True)
    if nz > 3:
        relay(3)
    lax.fori_loop(0, UP_ROWS, near, 0, unroll=True)

    def late_relay(k, _):
        relay(k)
        return 0

    lax.fori_loop(4, nz, late_relay, 0)

    def flat(x):
        if c_here % 16:
            return x.astype(F32).reshape(nz * c_here, HEAD_DIM).astype(BF16)
        return x.reshape(nz * c_here, HEAD_DIM)

    far_tile = tokens // 4

    def far(t, o, last):
        ids = pl.ds(pl.multiple_of(t * far_tile, 16), far_tile)
        col = (yi + o) % ny
        for h in range(heads):
            lo = h * HEAD_DIM
            ck = flat(ctx_all[col, :, :, lo:lo + HEAD_DIM])
            cv = flat(ctx_all[col, :, :, width + lo:width + lo + HEAD_DIM])
            s = dot_t(q[ids, lo:lo + HEAD_DIM], ck)
            mn = m_near[h, ids, :]
            m = jnp.maximum(jnp.max(s, axis=-1, keepdims=True), mn)
            e = jnp.exp2(s - m)
            w = jnp.exp2(mn - m)
            l = jnp.sum(e, axis=-1, keepdims=True) + w * l_near[h, ids, :]
            acc = dot(e.astype(BF16), cv) + w * o_near[ids, lo:lo + HEAD_DIM]
            if last:
                att[ids, lo:lo + HEAD_DIM] = (acc / l).astype(BF16)
            else:
                m_near[h, ids, :] = m
                l_near[h, ids, :] = l
                o_near[ids, lo:lo + HEAD_DIM] = acc

    def far_all(o, _):
        for t in range(4):
            far(t, o, False)
        return 0

    if ny > 1:
        far_all(0, 0)

    def settle_row(zb, _):
        def other(o, _):
            arrived(zb * ny + (yi + o) % ny)
            return 0

        lax.fori_loop(1, ny, other, 0)
        across(zb, sent)

        @pl.when(zb <= zi)
        def _():
            upward(zb, sent)

        @pl.when(zb >= zi)
        def _():
            downward(zb, sent)

        return 0

    lax.fori_loop(0, nz, settle_row, 0)

    lax.fori_loop(1, ny - 1, far_all, 0)

    def head_copy(src, dst):
        return pltpu.make_async_remote_copy(
            src_ref=att.at[pl.ds(pl.multiple_of(dst * own_n, 16), own_n)], dst_ref=own.at[src],
            send_sem=head_s.at[dst], recv_sem=head_r.at[src],
            device_id={"sp": sp, "tp": dst},
        )

    far((1 - my_half) * 2, ny - 1, True)
    far((1 - my_half) * 2 + 1, ny - 1, True)

    def send_other(j, _):
        head_copy(tp, (1 - my_half) * half_t + j).start()
        return 0

    lax.fori_loop(0, half_t, send_other, 0)
    far(my_half * 2, ny - 1, True)
    far(my_half * 2 + 1, ny - 1, True)

    def mate(o):
        return my_half * half_t + (tp + o) % half_t

    def send_same(o, _):
        head_copy(tp, mate(o)).start()
        return 0

    lax.fori_loop(1, half_t, send_same, 0)

    def wait_gate(o, _):
        tp_copy(gater, gate_s, gate_r, o).wait()
        return 0

    lax.fori_loop(1, nt, wait_gate, 0)
    gsum = gater[0]
    for i in range(1, nt):
        gsum = gsum + gater[i]
    gates = jnp.concatenate([gsum[j:j + 1] for j in range(8)], axis=1)
    loads[8].wait()
    own[tp] = att[pl.ds(pl.multiple_of(tp * own_n, 16), own_n), :]

    def settle(o, _):
        p = (tp + o) % nt
        head_copy(tp, p).wait_send()
        head_copy(p, p).wait_recv()
        return 0

    lax.fori_loop(1, nt, settle, 0)
    a = jnp.concatenate([own[i] for i in range(nt)], axis=1)
    my_rows = pl.ds(pl.multiple_of(tp * own_n, 16), own_n)
    for n0 in range(0, d, 512):
        y = dot(a, wo[:, n0:n0 + 512])
        out[:, n0:n0 + 512] = (
            lat[my_rows, n0:n0 + 512].astype(F32) + gates[:, n0:n0 + 512] * y
        ).astype(BF16)


def shards(
    ns, nt,
    latents, cond, ctx_cond, context, norm_gain, shift_weight, scale_weight, gate_weight,
    q_weight, k_weight, v_weight, out_weight, rel_bias,
):
    tokens, d = latents.shape
    c_here = context.shape[0]
    kt = shift_weight.shape[0]
    width = q_weight.shape[1]
    heads = width // HEAD_DIM
    own_n = tokens // nt
    table = jnp.transpose(rel_bias, (1, 0, 2))
    ny = 1
    while ns % (2 * ny) == 0 and 4 * ny * ny <= ns:
        ny *= 2
    halo = (UP_ROWS + DOWN_ROWS) * GRID_W
    vmem = pl.BlockSpec(memory_space=pltpu.VMEM)
    hbm = pl.BlockSpec(memory_space=pltpu.HBM)
    sem = pltpu.SemaphoreType.DMA
    return pl.pallas_call(
        functools.partial(kernel, ns, nt, ny),
        out_shape=jax.ShapeDtypeStruct((own_n, d), BF16),
        in_specs=[hbm] * 13,
        out_specs=vmem,
        scratch_shapes=[
            pltpu.VMEM((tokens, d), BF16),
            pltpu.VMEM((c_here, d), BF16),
            pltpu.VMEM((kt, d), BF16),
            pltpu.VMEM((kt, d), BF16),
            pltpu.VMEM((kt, d), BF16),
            pltpu.VMEM((d, 3 * width), BF16),
            pltpu.VMEM(out_weight.shape, BF16),
            pltpu.VMEM((nt, 8, d // 2), F32),
            pltpu.VMEM((nt, 8, d // 8), F32),
            pltpu.VMEM((8, d), F32),
            pltpu.VMEM((ny, ns // ny, c_here, 2 * width), BF16),
            pltpu.VMEM((tokens + halo, 2 * width), BF16),
            pltpu.VMEM((tokens, width), BF16),
            pltpu.VMEM((heads, 2 * WIN_ROWS - 2, GRID_W, PAIR), F32),
            pltpu.VMEM((tokens, width), F32),
            pltpu.VMEM((heads, tokens, 1), F32),
            pltpu.VMEM((heads, tokens, 1), F32),
            pltpu.VMEM((tokens, width), BF16),
            pltpu.VMEM((nt, own_n, width), BF16),
            pltpu.VMEM((2 * WIN_ROWS - 1, heads, PAIR), F32),
            pltpu.VMEM((1, d), F32),
            pltpu.VMEM((1, d), F32),
            pltpu.VMEM((1, d), F32),
            pltpu.VMEM(table.shape, F32),
            sem((13,)),
            sem((nt,)), sem((nt,)), sem((nt,)), sem((nt,)),
            sem((ny + 1, ns // ny)), sem((ns,)),
            sem((2,)), sem((2,)),
            sem((nt,)), sem((nt,)),
        ],
        compiler_params=pltpu.CompilerParams(
            collective_id=0, has_side_effects=True, vmem_limit_bytes=VMEM_BYTES - own_n * d * 2 - 300 * 1024
        ),
    )(
        cond[None], ctx_cond[None], norm_gain[None], table, latents, context, shift_weight, scale_weight, gate_weight,
        q_weight, k_weight, v_weight, out_weight,
    )


def solution(mesh):
    in_specs = (
        P("sp", None),
        P(),
        P(),
        P("sp", None),
        P(),
        P("tp", None),
        P("tp", None),
        P("tp", None),
        P(None, "tp"),
        P(None, "tp"),
        P(None, "tp"),
        P(),
        P("tp", None, None),
    )
    body = functools.partial(shards, mesh.shape["sp"], mesh.shape["tp"])
    return jax.shard_map(
        body, mesh=mesh, in_specs=in_specs, out_specs=P(("sp", "tp"), None), check_vma=False
    )
```
